32 devices in a mesh: kv: 4 (over z), tp: 8 (over y, x, core).
Axes of the slice: x: 2, y: 2, z: 4, core: 2. Of those that a mesh axis runs over, the one named last changes fastest.
Arguments:
- piece_tokens: bfloat16 [512, 2048], P('kv'), may hold values from -6 to 6
- dec_tokens: bfloat16 [8, 2048], P('kv'), may hold values from -6 to 6
- norm_gain: float32 [2048], replicated, may hold values from 0.1 to 1.9
- w_query_nope: bfloat16 [2048, 2048], P(None, 'tp'), may hold values from -0.125 to 0.125
- w_query_rope: bfloat16 [2048, 1024], P(None, 'tp'), may hold values from -0.125 to 0.125
- w_latent: bfloat16 [2048, 512], replicated, may hold values from -0.125 to 0.125
- w_key_rope: bfloat16 [2048, 64], replicated, may hold values from -0.125 to 0.125
- latent_gain: float32 [512], replicated, may hold values from 0.1 to 1.9
- w_key_up: bfloat16 [16, 128, 512], P('tp'), may hold values from -0.5 to 0.5
- w_value_up: bfloat16 [16, 512, 128], P('tp'), may hold values from -3 to 3
- w_out: bfloat16 [2048, 2048], P(None, 'tp'), may hold values from -0.25 to 0.25
- prompt_latent: bfloat16 [2048, 512], P('kv'), may hold values from -210 to 210
- prompt_rope: bfloat16 [2048, 64], P('kv'), may hold values from -6 to 6
- dec_latent: bfloat16 [8, 1024, 512], P('kv'), may hold values from -210 to 210
- dec_rope: bfloat16 [8, 1024, 64], P('kv'), may hold values from -6 to 6
- dec_lengths: int32 [8], P('kv'), may hold values from 1 to 1024, 4096 in all
Outputs:
- piece_out: bfloat16 [512, 2048], P('kv', 'tp')
- dec_out: bfloat16 [8, 2048], P('kv', 'tp')
The draws below stay inside these ranges and needn't reach their ends.
Inputs may be any that keep to these rules, and one draw needn't show every extreme that they name: `dec_lengths`: every decoding sequence has at least one live cache slot, and some sequence has all 1024.
All inputs are finite; a program needn't handle non-finite values. No bound on the sum of `dec_lengths` on one device may be relied on, other than what follows from the above.
Results may differ from the reference program's by a relative error of at most 0.025.
Values may be sent and summed in bfloat16 or wider, within the bound.
A program may use at most 128 MiB of HBM per device.

```python
import math
import jax
import jax.numpy as jnp
import numpy as np
from jax import lax

D = 2048
HEADS = 16
NOPE = 128
ROPE = 64
VDIM = 128
LATENT = 512
PIECE_DEV = 128
CTX_DEV = 512
DEC_CTX = 1024
PIECE = 512
CTX = 2048
DEC = 8
N_KV = 4


def drawn(key, shape):
    base_key = jax.random.fold_in(key, 0)
    return jnp.clip(jax.random.normal(base_key, shape, jnp.float32), -6.0, 6.0)


def draw_prompt_latent(key, part):
    return drawn(jax.random.fold_in(key, 11), (CTX, LATENT)).astype(jnp.bfloat16)


def draw_dec_latent(key, part):
    return drawn(jax.random.fold_in(key, 12), (DEC, DEC_CTX, LATENT)).astype(jnp.bfloat16)


def block_levels(own_key, dims, shards, least, largest):
    level = 1.0
    for dim, blocks in shards:
        steps = jax.random.uniform(jax.random.fold_in(jax.random.fold_in(own_key, 6), dim), (blocks,), jnp.float32, least / len(shards), largest / len(shards))
        level = level * jnp.repeat(jnp.exp(steps), dims[dim] // blocks).reshape((-1,) + (1,) * (len(dims) - 1 - dim))
    return level


def split_up(amount, total, limit, skew):
    portions = [(1 << 20) // math.isqrt(rank ** skew) + 1 for rank in range(2, amount + 1)]
    surplus, holding = total - limit - (amount - 1), [1] * (amount - 1)
    while surplus > 0:
        free = [i for i in range(amount - 1) if holding[i] < limit]
        pool, remaining = sum([portions[i] for i in free]), surplus
        for i in free:
            more = min(limit - holding[i], max(1, remaining * portions[i] // pool), surplus)
            holding[i] = holding[i] + more
            surplus = surplus - more
    return np.array([limit] + holding)


def ragged_sizes(rng, number_of, total, limit, slope):
    if number_of == 2:
        one = jax.random.randint(rng, (), max(1, total - limit), min(limit, total - 1) + 1)
        return jnp.stack([one, total - one])
    tallies = jnp.asarray(split_up(number_of, total, limit, slope), jnp.int32)
    pairs = (number_of - 1) // 2
    donor, receiver = tallies[1:1 + 2 * pairs:2], tallies[2:2 + 2 * pairs:2]
    slack = jnp.minimum(donor - 1, limit - receiver)
    shifted = jax.random.randint(jax.random.fold_in(rng, 1), (pairs,), 0, 1 << 20) % (slack + 1)
    tallies = tallies.at[1:1 + 2 * pairs:2].set(donor - shifted).at[2:2 + 2 * pairs:2].set(receiver + shifted)
    return tallies[jax.random.permutation(jax.random.fold_in(rng, 2), number_of)]


def bell_draw(key, extent, deviation, reach, cuts=(), held_as=jnp.bfloat16):
    gain = block_levels(key, extent, cuts, -0.22, 0.18) if cuts else 1.0
    values = jax.random.normal(key, extent, jnp.float32) * deviation * gain
    return jnp.minimum(jnp.maximum(values, -reach), reach).astype(held_as)


def setup_inputs(seed: int = 0) -> dict:
    splits = jax.random.split(jax.random.key(seed), 17)
    return {
        "piece_tokens": bell_draw(splits[0], (PIECE, D), 1.0, 6.0, ((0, 4),)),
        "dec_tokens": bell_draw(splits[1], (DEC, D), 1.0, 6.0, ((0, 4),)),
        "norm_gain": jnp.clip(1.0 + 0.18 * jax.random.normal(splits[2], (D,), jnp.float32), 0.1, 1.9),
        "w_query_nope": bell_draw(splits[3], (D, HEADS * NOPE), D ** -0.5, 0.125, ((1, 8),)),
        "w_query_rope": bell_draw(splits[4], (D, HEADS * ROPE), D ** -0.5, 0.125, ((1, 8),)),
        "w_latent": bell_draw(splits[5], (D, LATENT), D ** -0.5, 0.125),
        "w_key_rope": bell_draw(splits[6], (D, ROPE), D ** -0.5, 0.125),
        "latent_gain": jnp.clip(1.0 + 0.18 * jax.random.normal(splits[7], (LATENT,), jnp.float32), 0.1, 1.9),
        "w_key_up": bell_draw(splits[8], (HEADS, NOPE, LATENT), NOPE ** -0.5, 0.5, ((0, 8),)),
        "w_value_up": bell_draw(splits[9], (HEADS, LATENT, VDIM), 4 ** -0.5, 3.0, ((0, 8),)),
        "w_out": bell_draw(splits[10], (HEADS * VDIM, D), (HEADS * VDIM // 4) ** -0.5, 0.25, ((1, 8),)),
        "prompt_latent": draw_prompt_latent(jax.random.fold_in(splits[16], 71), 0),
        "prompt_rope": bell_draw(splits[12], (CTX, ROPE), 1.0, 6.0, ((0, 4),)),
        "dec_latent": draw_dec_latent(jax.random.fold_in(splits[16], 71), 0),
        "dec_rope": bell_draw(splits[14], (DEC, DEC_CTX, ROPE), 1.0, 6.0, ((0, 4),)),
        "dec_lengths": ragged_sizes(splits[15], DEC, DEC * DEC_CTX // 2, DEC_CTX, 2).astype(jnp.int32),
    }


epsilon = 1e-06
rope_base = 10000.0
masked = -1e+30

def normalize(values, gain_vec):
    mean_sq = lax.optimization_barrier(jnp.mean(values * values, axis=-1, keepdims=True))
    return values * lax.rsqrt(mean_sq + epsilon) * gain_vec

def rotate(values, positions):
    half_dim = values.shape[-1] // 2
    frequency = rope_base ** (-jnp.arange(half_dim, dtype=jnp.float32) / half_dim)
    angles = (positions.astype(jnp.float32)[:, None] * frequency[None, :])[:, None, :]
    cosines = jnp.cos(angles)
    sine_values = jnp.sin(angles)
    front_half = values[..., :half_dim]
    back_half = values[..., half_dim:]
    return jnp.concatenate([front_half * cosines - back_half * sine_values, front_half * sine_values + back_half * cosines], axis=-1)

def rounded(values):
    return lax.optimization_barrier(values.astype(jnp.bfloat16)).astype(jnp.float32)

def project(tokens, positions, norm_gain, w_query_nope, w_query_rope, w_latent, w_key_rope, latent_gain):
    row_count = tokens.shape[0]
    rope_dim = w_key_rope.shape[1]
    head_count = w_query_rope.shape[1] // rope_dim
    normed = normalize(tokens.astype(jnp.float32), norm_gain).astype(jnp.bfloat16)
    query_nope = jnp.dot(normed, w_query_nope, preferred_element_type=jnp.float32).astype(jnp.bfloat16)
    query_raw = jnp.dot(normed, w_query_rope, preferred_element_type=jnp.float32).reshape(row_count, head_count, rope_dim)
    query_rot = rotate(query_raw, positions).astype(jnp.bfloat16)
    latent = normalize(jnp.dot(normed, w_latent, preferred_element_type=jnp.float32), latent_gain).astype(jnp.bfloat16)
    key_raw = jnp.dot(normed, w_key_rope, preferred_element_type=jnp.float32)[:, None, :]
    key_rot = rotate(key_raw, positions)[:, 0].astype(jnp.bfloat16)
    return (query_nope, query_rot, latent, key_rot)

def absorb(query_nope, w_key_up):
    head_count, nope_dim, _ = w_key_up.shape
    by_head = query_nope.reshape(query_nope.shape[0], head_count, nope_dim)
    return jnp.einsum('nhd,hdc->nhc', by_head.astype(jnp.float32), w_key_up.astype(jnp.float32)).astype(jnp.bfloat16)

def reference(piece_tokens, dec_tokens, norm_gain, w_query_nope, w_query_rope, w_latent, w_key_rope, latent_gain, w_key_up, w_value_up, w_out, prompt_latent, prompt_rope, dec_latent, dec_rope, dec_lengths):
    score_scale = (NOPE + ROPE) ** (-0.5)
    weights_args = (norm_gain, w_query_nope, w_query_rope, w_latent, w_key_rope, latent_gain)
    piece_pos = CTX + jnp.arange(PIECE, dtype=jnp.int32)
    query_nope, query_rot, new_latent, new_rot = project(piece_tokens, piece_pos, *weights_args)
    query_lat = absorb(query_nope, w_key_up)
    key_count = CTX_DEV + PIECE_DEV
    key_latent = jnp.concatenate([prompt_latent.reshape(N_KV, CTX_DEV, LATENT), new_latent.reshape(N_KV, PIECE_DEV, LATENT)], axis=1)
    key_rot = jnp.concatenate([prompt_rope.reshape(N_KV, CTX_DEV, ROPE), new_rot.reshape(N_KV, PIECE_DEV, ROPE)], axis=1)
    flat_latent = key_latent.reshape(N_KV * key_count, LATENT)
    flat_rot = key_rot.reshape(N_KV * key_count, ROPE)
    column = jnp.arange(N_KV * key_count, dtype=jnp.int32)
    inner_pos = column % key_count
    piece_place = column // key_count * PIECE_DEV + inner_pos - CTX_DEV
    query_place = jnp.arange(PIECE, dtype=jnp.int32)
    visible = (inner_pos[None, :] < CTX_DEV) | (piece_place[None, :] <= query_place[:, None])
    latent_f32 = key_latent.astype(jnp.float32)

    def one_head(head_args):
        head_lat, head_rot, w_value = head_args
        scores = (jnp.dot(head_lat, flat_latent.T, preferred_element_type=jnp.float32) + jnp.dot(head_rot, flat_rot.T, preferred_element_type=jnp.float32)) * score_scale
        scores = jnp.where(visible, scores, masked)
        row_peak = lax.optimization_barrier(jnp.max(scores, axis=1, keepdims=True))
        weights = jnp.exp(scores - row_peak)
        weight_sum = lax.optimization_barrier(jnp.sum(weights, axis=1))
        blocks = rounded(weights).reshape(PIECE, N_KV, key_count)
        mixed_lat = jnp.einsum('qjk,jkc->jqc', blocks, latent_f32).astype(jnp.bfloat16)
        mixed_lat = lax.optimization_barrier(mixed_lat)
        block_parts = rounded(jnp.einsum('jqc,cv->jqv', mixed_lat.astype(jnp.float32), w_value.astype(jnp.float32)))
        summed = lax.optimization_barrier(jnp.sum(block_parts, axis=0))
        return (summed / weight_sum[:, None]).astype(jnp.bfloat16)
    piece_heads = lax.map(one_head, (query_lat.transpose(1, 0, 2), query_rot.transpose(1, 0, 2), w_value_up))
    piece_attn = piece_heads.transpose(1, 0, 2).reshape(PIECE, -1)
    dec_nope, dec_rot, own_lat, own_rot = project(dec_tokens, dec_lengths, *weights_args)
    dec_query = absorb(dec_nope, w_key_up).astype(jnp.float32)
    dec_rotf = dec_rot.astype(jnp.float32)
    cache_lat = dec_latent.astype(jnp.float32)
    cache_scores = (jnp.einsum('bhc,bkc->bhk', dec_query, cache_lat) + jnp.einsum('bhr,bkr->bhk', dec_rotf, dec_rope.astype(jnp.float32))) * score_scale
    live_keys = jnp.arange(dec_latent.shape[1], dtype=jnp.int32)[None, None, :] < dec_lengths[:, None, None]
    cache_scores = jnp.where(live_keys, cache_scores, masked)
    own_scores = (jnp.einsum('bhc,bc->bh', dec_query, own_lat.astype(jnp.float32)) + jnp.einsum('bhr,br->bh', dec_rotf, own_rot.astype(jnp.float32))) * score_scale
    dec_peak = jnp.maximum(lax.optimization_barrier(jnp.max(cache_scores, axis=2)), own_scores)
    cache_w = jnp.exp(cache_scores - dec_peak[:, :, None])
    own_w = jnp.exp(own_scores - dec_peak)
    dec_sum = lax.optimization_barrier(jnp.sum(cache_w, axis=2)) + own_w
    dec_mix = (jnp.einsum('bhk,bkc->bhc', rounded(cache_w), cache_lat) + rounded(own_w)[:, :, None] * own_lat.astype(jnp.float32)[:, None, :]).astype(jnp.bfloat16)
    dec_mix = lax.optimization_barrier(dec_mix)
    dec_value = rounded(jnp.einsum('bhc,hcv->bhv', dec_mix.astype(jnp.float32), w_value_up.astype(jnp.float32)))
    dec_attn = (dec_value / dec_sum[:, :, None]).astype(jnp.bfloat16).reshape(DEC, -1)
    piece_out = jnp.dot(piece_attn, w_out, preferred_element_type=jnp.float32).astype(jnp.bfloat16)
    dec_out = jnp.dot(dec_attn, w_out, preferred_element_type=jnp.float32).astype(jnp.bfloat16)
    return (piece_out, dec_out)
```

```python
import functools

import jax
import jax.numpy as jnp
import numpy as np
from jax import lax
from jax.experimental import pallas as pl
from jax.experimental.pallas import tpu as pltpu
from jax.sharding import PartitionSpec as P

epsilon = 1e-06
rope_base = 10000.0
masked = -1e30
F32 = jnp.float32
BF16 = jnp.bfloat16


def dot(a, b):
    return jnp.dot(a, b, preferred_element_type=F32)


def dot_t(a, b):
    return lax.dot_general(a, b, (((1,), (1,)), ((), ())), preferred_element_type=F32)


def normalize(values, gain_vec):
    mean_sq = jnp.mean(values * values, axis=-1, keepdims=True)
    return values * lax.rsqrt(mean_sq + epsilon) * gain_vec


def kernel(n_kv, n_tp, heads, pad, *refs):
    (
        lengths_hbm, freq_hbm, gain_hbm, lgain_hbm, dec_tok_hbm,
        tok_hbm, wqn_hbm, wqr_hbm, wlat_hbm, wkr_hbm, wku_hbm, wvu_hbm, wout_hbm,
        plat_hbm, prope_hbm, dlat_hbm, drope_hbm,
        out_ref, dec_out_ref,
        lengths, freq_ref, gain_ref, lgain_ref, dec_tok_ref,
        tok, wqn, wqr, wlat, wkr, wku, wvu, wout, klat, prope, dlat, drope,
        normed, krot, qbuf, obuf, ostat, pbuf, sbuf, att,
        load_sem, q_send, q_recv, p_send, p_recv, s_send, s_recv, d_send, d_recv, a_send, a_recv,
        f_send,
    ) = refs
    rows = tok.shape[0]
    cached = plat_hbm.shape[0]
    latent_dim = wlat.shape[1]
    rope = wkr_hbm.shape[0]
    nope = wku.shape[1]
    vdim = wvu.shape[2]
    dec_rows = dec_tok_ref.shape[0]
    dec_keys = dlat.shape[1]
    nope_width = heads * nope
    rot_width = heads * rope
    scale = (nope + rope) ** (-0.5)
    me = lax.axis_index("kv")
    my_t = lax.axis_index("tp")

    loads = {}
    copies = range(heads)
    band = [pl.ds(h * rope, rope) for h in copies]
    sources = (
        ("small", [(freq_hbm, freq_ref), (gain_hbm, gain_ref), (dec_tok_hbm, dec_tok_ref)]),
        ("lengths", [(lengths_hbm, lengths)]), ("tok", [(tok_hbm, tok)]), ("wqn", [(wqn_hbm, wqn)]), ("wqr", [(wqr_hbm, wqr)]),
        ("wlat", [(wlat_hbm, wlat)]), ("lgain", [(lgain_hbm, lgain_ref)]), ("wkr", [(wkr_hbm, wkr.at[band[h]]) for h in copies]),
        ("prope", [(prope_hbm, prope.at[band[h]]) for h in copies]),
        ("plat", [(plat_hbm, klat.at[pl.ds(0, cached)])]), ("wku", [(wku_hbm, wku)]),
        ("wvu", [(wvu_hbm, wvu)]), ("dlat", [(dlat_hbm, dlat)]),
        ("drope", [(drope_hbm, drope.at[:, band[h]]) for h in copies]),
        ("wout", [(wout_hbm, wout)]),
    )
    count = 0
    for name, pairs in sources:
        loads[name] = []
        for src, dst in pairs:
            loads[name].append(pltpu.make_async_copy(src, dst, load_sem.at[count]))
            loads[name][-1].start()
            count += 1

    def loaded(name):
        for copy in loads[name]:
            copy.wait()

    barrier = pltpu.get_barrier_semaphore()
    for d in range(1, n_kv):
        pl.semaphore_signal(
            barrier, inc=1, device_id={"kv": lax.rem(me + d, n_kv)},
            device_id_type=pl.DeviceIdType.MESH,
        )
    for d in range(1, n_tp):
        pl.semaphore_signal(
            barrier, inc=1, device_id={"tp": lax.rem(my_t + d, n_tp)},
            device_id_type=pl.DeviceIdType.MESH,
        )

    def remote(src, dst, send, recv, axis, target):
        return pltpu.make_async_remote_copy(
            src_ref=src, dst_ref=dst, send_sem=send, recv_sem=recv,
            device_id={axis: target}, device_id_type=pl.DeviceIdType.MESH,
        )

    loaded("small")
    loaded("lengths")
    row = lax.broadcasted_iota(jnp.int32, (rows + pad, rot_width), 0)
    position = n_kv * cached + me * rows + row
    for b in range(dec_rows):
        position = jnp.where(row == rows + b, lengths[b], position)
    angles = position.astype(F32) * freq_ref[...]
    lane = lax.broadcasted_iota(jnp.int32, (rows + pad, rot_width), 1)
    front = lane % rope < rope // 2
    cosines = jnp.cos(angles)
    sines = jnp.sin(angles)
    sines = jnp.where(front, -sines, sines)

    gain = gain_ref[...]
    normed[pl.ds(rows, pad), :] = jnp.zeros((pad, normed.shape[1]), BF16)
    dec_norm = normalize(dec_tok_ref[...].astype(F32), gain).astype(BF16)
    normed[pl.ds(rows, dec_rows), :] = dec_norm
    loaded("tok")
    normed[pl.ds(0, rows), :] = normalize(tok[...].astype(F32), gain).astype(BF16)

    def rotated(v):
        half = rope // 2
        swapped = jnp.where(
            front, pltpu.roll(v, rot_width - half, 1), pltpu.roll(v, half, 1)
        )
        return (v * cosines + swapped * sines).astype(BF16)

    x = normed[...]
    loaded("wqn")
    q_nope = dot(x, wqn[...]).astype(BF16)
    loaded("wqr")
    q_rot = rotated(dot(x, wqr[...]))
    qbuf[me, :, 0:nope_width] = q_nope[:rows]
    qbuf[me, :, nope_width:] = q_rot[:rows]

    pl.semaphore_wait(barrier, n_kv + n_tp - 2)

    chunks = q_send.shape[1]
    chunk = rows // chunks
    line = n_kv == 4

    def q_copy(block, target, slot, c):
        part = qbuf.at[block, pl.ds(c * chunk, chunk)]
        return remote(part, part, q_send.at[slot, c], q_recv.at[block, c], "kv", target)

    def q_arrived(block):
        for c in range(chunks):
            q_copy(block, lax.rem(me + 1, n_kv), 0, c).wait_recv()

    upper = me // 2
    middle = lax.rem(me + upper, 2) == 1
    own_end, far_end = 3 * upper, 3 - 3 * upper
    own_middle, far_middle = 1 + upper, 2 - upper
    if line:
        first = jnp.where(middle, far_middle, own_middle)
        second = jnp.where(middle, own_end, far_middle)
        first_served = jnp.where(middle, far_middle, own_middle)
        second_served = jnp.where(middle, far_end, far_middle)
        last_served = jnp.where(middle, own_end, far_end)
        targets = [first, second]
    else:
        targets = [lax.rem(me + d, n_kv) for d in range(1, n_kv)]
    for i, target in enumerate(targets):
        for c in range(chunks):
            q_copy(me, target, i, c).start()

    def hand_on(block, slot):
        if line:
            @pl.when(middle)
            def _():
                for c in range(chunks):
                    q_copy(block, lax.rem(me + 1, n_kv), 0, c).wait_recv()
                    q_copy(block, own_end, slot, c).start()

    loaded("wlat")
    loaded("lgain")
    latent = normalize(dot(x, wlat[...]), lgain_ref[...]).astype(BF16)
    loaded("plat")
    klat[pl.ds(cached, rows), :] = latent[:rows]
    loaded("wkr")
    k_rot = rotated(dot_t(x, wkr[...]))
    krot[...] = k_rot[:rows]
    loaded("prope")
    loaded("wku")
    loaded("wvu")

    def stacked(nope_part, rot_part):
        count = nope_part.shape[0]
        lanes = lax.broadcasted_iota(jnp.int32, (count, rot_width), 1) // rope
        lat = [dot(nope_part[:, h * nope:(h + 1) * nope], wku[h]).astype(BF16) for h in range(heads)]
        rot = [jnp.where(lanes == h, rot_part, jnp.zeros_like(rot_part)) for h in range(heads)]
        return jnp.concatenate(lat, axis=0), jnp.concatenate(rot, axis=0)

    total = heads * rows
    stat_lane = lax.broadcasted_iota(jnp.int32, (total, 128), 1)
    query_row = lax.broadcasted_iota(jnp.int32, (total, rows), 0) % rows
    key_col = lax.broadcasted_iota(jnp.int32, (total, rows), 1)

    def attend(block, j):
        lat, rot = stacked(block[:, :nope_width], block[:, nope_width:])
        s_c = (dot_t(lat, klat[pl.ds(0, cached), :]) + dot(rot, prope[...])) * scale
        s_p = (
            dot_t(lat, klat[pl.ds(cached, rows), :]) + dot_t(rot, krot[...])
        ) * scale
        s_p = jnp.where(me * rows + key_col <= j * rows + query_row, s_p, masked)
        peak = jnp.maximum(
            jnp.max(s_c, axis=1, keepdims=True), jnp.max(s_p, axis=1, keepdims=True)
        )
        w_c = jnp.exp(s_c - peak)
        w_p = jnp.exp(s_p - peak)
        weight_sum = jnp.sum(w_c, axis=1, keepdims=True) + jnp.sum(w_p, axis=1, keepdims=True)
        mixed = (
            dot(w_c.astype(BF16), klat[pl.ds(0, cached), :])
            + dot(w_p.astype(BF16), klat[pl.ds(cached, rows), :])
        ).astype(BF16)
        values = [
            dot(mixed[h * rows:(h + 1) * rows], wvu[h]).astype(BF16) for h in range(heads)
        ]
        stat = jnp.where(stat_lane == 0, peak, jnp.where(stat_lane == 1, weight_sum, 0.0))
        return values, jnp.transpose(stat)[0:2]

    def store(values, stat, value_ref, stat_ref, slot):
        for h in range(heads):
            value_ref[slot, h] = values[h]
        stat_ref[slot] = stat

    values, stat = attend(qbuf[me], me)
    store(values, stat, pbuf, sbuf, me)

    loaded("dlat")
    loaded("drope")
    d_lat, d_rot = stacked(q_nope[rows:], q_rot[rows:])
    own_lat = jnp.concatenate([latent[rows:]] * heads, axis=0).astype(F32)
    own_rot = jnp.concatenate([k_rot[rows:]] * heads, axis=0).astype(F32)
    own_s = (
        jnp.sum(d_lat.astype(F32) * own_lat, axis=1, keepdims=True)
        + jnp.sum(d_rot.astype(F32) * own_rot, axis=1, keepdims=True)
    ) * scale
    row_of = lax.broadcasted_iota(jnp.int32, (heads * pad, 1), 0) % pad
    key_at = lax.broadcasted_iota(jnp.int32, (heads * pad, dec_keys), 1)
    mix = jnp.zeros((heads * pad, latent_dim), F32)
    d_sum = jnp.ones((heads * pad, 1), F32)
    for b in range(dec_rows):
        keys = dlat[b]
        s = (dot_t(d_lat, keys) + dot(d_rot, drope[b])) * scale
        s = jnp.where(key_at < lengths[b], s, masked)
        peak = jnp.maximum(jnp.max(s, axis=1, keepdims=True), own_s)
        w = jnp.exp(s - peak)
        own_w = jnp.exp(own_s - peak)
        mix_b = dot(w.astype(BF16), keys) + own_w.astype(BF16).astype(F32) * own_lat
        sum_b = jnp.sum(w, axis=1, keepdims=True) + own_w
        if b < 2:
            hand_on((far_middle, far_end)[b], 2 + b)
        mix = jnp.where(row_of == b, mix_b, mix)
        d_sum = jnp.where(row_of == b, sum_b, d_sum)
    for b in range(dec_rows, 2):
        hand_on((far_middle, far_end)[b], 2 + b)
    mix = mix.astype(BF16)
    for h in range(heads):
        part = slice(h * pad, (h + 1) * pad)
        d_value = dot(mix[part], wvu[h]).astype(BF16).astype(F32)
        att[my_t, pl.ds(rows, pad), h * vdim:(h + 1) * vdim] = (d_value / d_sum[part]).astype(BF16)

    paired = n_tp == 8
    if paired:
        tp_order = [6, 7, 2, 4, 3, 5, 1]
        head_order = [6, 2, 4, 1]
        relayed = [2, 4, 6]
    else:
        tp_order = list(range(1, n_tp))
        head_order = tp_order
        relayed = []

    def tp_peer(d):
        if n_tp != 8:
            return lax.rem(my_t + d, n_tp)
        high, mid, low = my_t // 4, my_t // 2, my_t
        return (
            lax.rem(high + d // 4, 2) * 4 + lax.rem(mid + d // 2 % 2, 2) * 2 + lax.rem(low + d % 2, 2)
        )

    def dec_part(t):
        return att.at[t, pl.ds(rows, pad), :]

    def head_part(t, h):
        return att.at[t, pl.ds(0, rows), pl.ds(h * vdim, vdim)]

    def dec_copy(d):
        part = dec_part(my_t)
        return remote(part, part, d_send.at[d], d_recv.at[my_t], "tp", tp_peer(d))

    def head_copy(d, h):
        part = head_part(my_t, h)
        return remote(part, part, a_send.at[d, h], a_recv.at[my_t, h], "tp", tp_peer(d))

    def relay_copy(d, h):
        part = head_part(tp_peer(d), h)
        return remote(part, part, f_send.at[d, h], a_recv.at[tp_peer(d), h], "tp", tp_peer(1))

    for d in tp_order:
        dec_copy(d).start()

    def p_copies(j):
        return [remote(ostat.at[j], sbuf.at[me], s_send.at[j], s_recv.at[me], "kv", j)] + [
            remote(obuf.at[j, h], pbuf.at[me, h], p_send.at[j, h], p_recv.at[me, h], "kv", j)
            for h in range(heads)
        ]

    def serve(j):
        values, stat = attend(qbuf[j], j)
        store(values, stat, obuf, ostat, j)
        for copy in p_copies(j):
            copy.start()

    def serve_at(d):
        j = lax.rem(me + d, n_kv)
        q_arrived(j)
        serve(j)

    if line:
        pl.when(jnp.logical_not(middle))(lambda: q_arrived(own_middle))
        serve(first_served)
        pl.when(jnp.logical_not(middle))(lambda: q_arrived(far_middle))
        serve(second_served)
        q_arrived(last_served)
        serve(last_served)
    else:
        lax.fori_loop(1, n_kv, lambda d, c: (serve_at(d), c)[1], 0)

    for d in range(1, n_kv):
        j = lax.rem(me + d, n_kv)
        remote(ostat.at[j], sbuf.at[j], s_send.at[j], s_recv.at[j], "kv", j).wait_recv()

    peak = sbuf[0, 0:1, :]
    for j in range(1, n_kv):
        peak = jnp.maximum(peak, sbuf[j, 0:1, :])
    factors = [jnp.exp(sbuf[j, 0:1, :] - peak) for j in range(n_kv)]
    whole = factors[0] * sbuf[0, 1:2, :]
    for j in range(1, n_kv):
        whole = whole + factors[j] * sbuf[j, 1:2, :]
    table_row = lax.broadcasted_iota(jnp.int32, (128, total), 0)
    table = jnp.zeros((128, total), F32)
    for j in range(n_kv):
        table = jnp.where(table_row == j, factors[j] / whole, table)
    table = jnp.transpose(table)
    for h in range(heads):
        for d in range(1, n_kv):
            j = lax.rem(me + d, n_kv)
            remote(
                obuf.at[j, h], pbuf.at[j, h], p_send.at[j, h], p_recv.at[j, h], "kv", j
            ).wait_recv()
        acc = jnp.zeros((rows, vdim), F32)
        for j in range(n_kv):
            column = table[h * rows:(h + 1) * rows, j:j + 1]
            acc = acc + column * pbuf[j, h].astype(F32)
        att[my_t, pl.ds(0, rows), h * vdim:(h + 1) * vdim] = acc.astype(BF16)
        for d in head_order:
            head_copy(d, h).start()

    loaded("wout")
    width = heads * vdim

    def project_out(t):
        return dot(att[t], wout[pl.ds(pl.multiple_of(t * width, width), width), :])

    def head_arrived(d, h):
        part = head_part(tp_peer(d), h)
        remote(part, part, a_send.at[d, h], a_recv.at[tp_peer(d), h], "tp", tp_peer(d)).wait_recv()

    result = project_out(my_t)
    for h in range(heads):
        for d in relayed:
            head_arrived(d, h)
            relay_copy(d, h).start()
    for d in (relayed + [1, 3, 5, 7] if paired else reversed(tp_order)):
        t = tp_peer(d)
        part = dec_part(t)
        remote(part, part, d_send.at[d], d_recv.at[t], "tp", t).wait_recv()
        if d not in relayed:
            for h in range(heads):
                head_arrived(d, h)
        result = result + project_out(t)
    result = result.astype(BF16)
    out_ref[...] = result[:rows]
    dec_out_ref[...] = result[rows:rows + dec_rows]

    for i, target in enumerate(targets):
        for c in range(chunks):
            q_copy(me, target, i, c).wait_send()
    if line:
        @pl.when(middle)
        def _():
            for c in range(chunks):
                q_copy(far_middle, own_end, 2, c).wait_send()
                q_copy(far_end, own_end, 3, c).wait_send()
    for d in range(1, n_kv):
        for copy in p_copies(lax.rem(me + d, n_kv)):
            copy.wait_send()
    for d in range(1, n_tp):
        dec_copy(d).wait_send()
        for h in range(heads):
            if d in head_order:
                head_copy(d, h).wait_send()
            if d in relayed:
                relay_copy(d, h).wait_send()


def deliver(piece, dec, piece_out, dec_out, sem):
    copies = [
        pltpu.make_async_copy(piece, piece_out, sem.at[0]),
        pltpu.make_async_copy(dec, dec_out, sem.at[1]),
    ]
    for copy in copies:
        copy.start()
    for copy in copies:
        copy.wait()


def shards(
    n_kv, n_tp,
    piece_tokens, dec_tokens, norm_gain, w_query_nope, w_query_rope, w_latent, w_key_rope,
    latent_gain, w_key_up, w_value_up, w_out, prompt_latent, prompt_rope, dec_latent, dec_rope,
    dec_lengths,
):
    rows, width = piece_tokens.shape
    dec_rows = dec_tokens.shape[0]
    pad = -(-dec_rows // 16) * 16
    cached, latent_dim = prompt_latent.shape
    heads, nope, _ = w_key_up.shape
    vdim = w_value_up.shape[2]
    rope = w_key_rope.shape[1]
    half = rope // 2
    frequency = rope_base ** (-np.arange(half) / half)
    frequency = jnp.asarray(np.tile(frequency, 2 * heads)[None, :].astype(np.float32))
    vmem = pl.BlockSpec(memory_space=pltpu.VMEM)
    anywhere = pl.BlockSpec(memory_space=pltpu.HBM)
    sem = pltpu.SemaphoreType.DMA
    scratch = [
        pltpu.SMEM(dec_lengths.shape, jnp.int32),
        pltpu.VMEM(frequency.shape, F32),
        pltpu.VMEM((1, width), F32),
        pltpu.VMEM((1, latent_dim), F32),
        pltpu.VMEM(dec_tokens.shape, BF16),
        pltpu.VMEM(piece_tokens.shape, BF16),
        pltpu.VMEM(w_query_nope.shape, BF16),
        pltpu.VMEM(w_query_rope.shape, BF16),
        pltpu.VMEM(w_latent.shape, BF16),
        pltpu.VMEM((heads * rope, width), BF16),
        pltpu.VMEM(w_key_up.shape, BF16),
        pltpu.VMEM(w_value_up.shape, BF16),
        pltpu.VMEM(w_out.shape, BF16),
        pltpu.VMEM((cached + rows, latent_dim), BF16),
        pltpu.VMEM((heads * rope, cached), BF16),
        pltpu.VMEM(dec_latent.shape, BF16),
        pltpu.VMEM((dec_rows, heads * rope, dec_latent.shape[1]), BF16),
        pltpu.VMEM((rows + pad, width), BF16),
        pltpu.VMEM((rows, heads * rope), BF16),
        pltpu.VMEM((n_kv, rows, heads * (nope + rope)), BF16),
        pltpu.VMEM((n_kv, heads, rows, vdim), BF16),
        pltpu.VMEM((n_kv, 2, heads * rows), F32),
        pltpu.VMEM((n_kv, heads, rows, vdim), BF16),
        pltpu.VMEM((n_kv, 2, heads * rows), F32),
        pltpu.VMEM((n_tp, rows + pad, heads * vdim), BF16),
        sem((14 + 3 * heads,)),
    ] + (
        [sem((n_kv, 4))] * 2 + [sem((n_kv, heads))] * 2 + [sem((n_kv,))] * 2
        + [sem((n_tp,))] * 2 + [sem((n_tp, heads))] * 3
    )
    results = pl.pallas_call(
        functools.partial(kernel, n_kv, n_tp, heads, pad),
        out_shape=(
            pltpu.VMEM((rows, w_out.shape[1]), BF16),
            pltpu.VMEM((dec_rows, w_out.shape[1]), BF16),
        ),
        in_specs=[anywhere] * 17,
        out_specs=(vmem, vmem),
        scratch_shapes=scratch,
        compiler_params=pltpu.CompilerParams(
            collective_id=0, has_side_effects=True, vmem_limit_bytes=60 * 1024 * 1024
        ),
    )(
        dec_lengths, frequency, norm_gain[None, :], latent_gain[None, :], dec_tokens,
        piece_tokens, w_query_nope, w_query_rope, w_latent, w_key_rope.T, w_key_up, w_value_up,
        w_out, prompt_latent, prompt_rope.T, dec_latent, jnp.swapaxes(dec_rope, 1, 2),
    )
    return pl.pallas_call(
        deliver,
        out_shape=tuple(pltpu.HBM(r.shape, r.dtype) for r in results),
        in_specs=[vmem, vmem],
        out_specs=(anywhere, anywhere),
        scratch_shapes=[sem((2,))],
    )(*[pltpu.with_memory_space_constraint(r, pltpu.VMEM) for r in results])


def solution(mesh):
    in_specs = (
        P("kv", None),
        P("kv", None),
        P(),
        P(None, "tp"),
        P(None, "tp"),
        P(),
        P(),
        P(),
        P("tp", None, None),
        P("tp", None, None),
        P(None, "tp"),
        P("kv", None),
        P("kv", None),
        P("kv", None, None),
        P("kv", None, None),
        P("kv"),
    )
    out_specs = (P("kv", "tp"), P("kv", "tp"))
    body = functools.partial(shards, mesh.shape["kv"], mesh.shape["tp"])
    return jax.shard_map(body, mesh=mesh, in_specs=in_specs, out_specs=out_specs, check_vma=False)
```
